32 devices in a mesh: ep: 8 (over z, core), tp: 4 (over y, x).
Axes of the slice: x: 2, y: 2, z: 4, core: 2. Of those that a mesh axis runs over, the one named last changes fastest.
Arguments:
- tokens: bfloat16 [256, 2048], P('ep'), may hold values from -6 to 6
- recurrent_head_state: float32 [256, 16, 4096], P('ep', 'tp'), may hold values from -4 to 4
- first_norm_gain: float32 [2048], replicated, may hold values from 0.1 to 1.9
- receptance_matrix: bfloat16 [2048, 1024], P(None, 'tp'), may hold values from -0.125 to 0.125
- key_matrix: bfloat16 [2048, 1024], P(None, 'tp'), may hold values from -0.125 to 0.125
- value_matrix: bfloat16 [2048, 1024], P(None, 'tp'), may hold values from -0.125 to 0.125
- decay_matrix: bfloat16 [2048, 1024], P(None, 'tp'), may hold values from -0.125 to 0.125
- decay_offset: float32 [1024], P('tp'), may hold values from -3 to 0.5
- correction_offset: float32 [1024], P('tp'), may hold values from -2 to 2
- correction_key_factor: float32 [1024], P('tp'), may hold values from -1 to 1
- own_term_weight: float32 [1024], P('tp'), may hold values from -0.9 to 0.9
- head_norm_gain: float32 [1024], P('tp'), may hold values from 0.1 to 1.9
- output_matrix: bfloat16 [1024, 2048], P('tp'), may hold values from -0.1875 to 0.1875
- second_norm_gain: float32 [2048], replicated, may hold values from 0.1 to 1.9
- routing: int32 [256, 2], replicated, may hold values from 0 to 7, all different within a row; in each aligned block of 32 rows (0 to 31, 32 to 63, ...) at most 16 rows name the same one
- routing_weight: float32 [256, 2], P('ep'), may hold values from 0.1 to 1
- expert_gate_weight: bfloat16 [8, 2048, 4096], P('ep', None, 'tp'), may hold values from -0.125 to 0.125
- expert_up_weight: bfloat16 [8, 2048, 4096], P('ep', None, 'tp'), may hold values from -0.125 to 0.125
- expert_down_weight: bfloat16 [8, 4096, 2048], P('ep', 'tp'), may hold values from -0.125 to 0.125
- dense_gate_weight: bfloat16 [2048, 2816], P(None, 'ep'), may hold values from -0.125 to 0.125
- dense_up_weight: bfloat16 [2048, 2816], P(None, 'ep'), may hold values from -0.125 to 0.125
- dense_down_weight: bfloat16 [2816, 2048], P('ep'), may hold values from -0.109375 to 0.109375
- dense_gate_offset: float32 [2048], replicated, may hold values from -3 to 3
Outputs:
- layer_out: bfloat16 [256, 2048], P(('ep', 'tp'))
- next_state: float32 [256, 16, 4096], P('ep', 'tp')
The draws below stay inside these ranges and needn't reach their ends.
Inputs may be any that keep to these rules, and one draw needn't show every extreme that they name: `routing`: each row names 2 different experts. In each aligned block of 32 rows no expert is named more than 16 times, a bound that some block reaches.
All inputs are finite; a program needn't handle non-finite values.
Results may differ from the reference program's by a relative error of at most 0.017.
Values may be sent and summed in bfloat16 or wider, within the bound.
A program may use at most 64 MiB of HBM per device.

```python
import math
from functools import partial
import jax
import jax.numpy as jnp
import numpy as np
from jax import lax

D = 2048
HEAD_COUNT = 16
HEAD_WIDTH = 64
FF_E = 4096
FF_D = 2816
TOP_K = 2
B_DEV = 32
B_TOT = 256
EXPERTS = 8
CAP = 16
N_EP = 8


def strengthened(entries, rng, source, target, parts, factor):
    def block_of(axis_at):
        return (jnp.arange(entries.shape[axis_at]) // (entries.shape[axis_at] // parts)).reshape((-1,) + (1,) * (entries.ndim - 1 - axis_at))

    first = jax.random.permutation(rng, parts)[block_of(target)]
    second = (block_of(target) + parts // 2) % parts
    return jnp.where((block_of(source) == first) | (block_of(source) == second), factor * entries, entries)


def levels(rng, extent, pieces, smallest, high):
    level, own = 1.0, jax.random.fold_in(rng, 6)
    for position, blocks in pieces:
        draws = jnp.exp(jax.random.uniform(jax.random.fold_in(own, position), (blocks,), jnp.float32, smallest / len(pieces), high / len(pieces)))
        level = level * jnp.repeat(draws, extent[position] // blocks).reshape([-1 if axis == position else 1 for axis in range(len(extent))])
    return level


def shared_out(stream_key, own, number, rows, amount, top, most, lean):
    sequence = jax.random.permutation(stream_key, amount)
    crowded, common = shares(amount, rows * top, most, lean, True), shares(amount, rows * top, most, lean, False)
    places = jnp.arange(amount)

    def named(tallies, turn):
        used = int((tallies > 0).sum())
        fixed = max(1, used // 4)
        moved = fixed + (places - fixed + turn * (used - fixed)) % max(1, amount - fixed)
        return jnp.zeros((amount,), jnp.int32).at[sequence[jnp.where(places < fixed, places, moved)]].set(jnp.asarray(tallies, jnp.int32))

    tallies = jnp.where(number % 4 == 0, named(crowded, number // 4), named(common, number - number // 4 - 1))
    mixed = jax.random.permutation(jax.random.fold_in(own, 3), amount)
    giver, receiver = mixed[0:amount // 2 * 2:2], mixed[1:amount // 2 * 2:2]
    room = jnp.minimum(tallies[giver] - 1, most - tallies[receiver]) // 2
    room = jnp.where((giver == sequence[0]) | (receiver == sequence[0]) | (tallies[receiver] == 0), 0, jnp.maximum(room, 0))
    moved = jax.random.randint(jax.random.fold_in(own, 4), (amount // 2,), 0, 1 << 20) % (room + 1)
    tallies = tallies.at[giver].add(-moved).at[receiver].add(moved)
    labels = jnp.searchsorted(jnp.cumsum(tallies), jnp.arange(rows * top), side="right").astype(jnp.int32)
    listing = labels.reshape(top, rows).T
    listing = listing[jax.random.permutation(jax.random.fold_in(own, 1), rows)]
    turn = jax.random.randint(jax.random.fold_in(own, 2), (rows, 1), 0, top)
    return jnp.take_along_axis(listing, (jnp.arange(top)[None, :] + turn) % top, axis=1)


def shares(amount, total, reach, slope, full):
    weights = [(1 << 20) // math.isqrt(grade ** slope) + 1 for grade in range(1, amount + 1)]
    largest = reach if full else min(reach, max(-(-total // amount), total * weights[0] // sum(weights)))
    least = 1 if total - largest >= amount - 1 else 0
    counts, spare = [largest] + [least] * (amount - 1), total - largest - least * (amount - 1)
    while spare > 0:
        movable = [i for i in range(1, amount) if counts[i] < largest] or [i for i in range(1, amount) if counts[i] < reach]
        pool, left = sum([weights[i] for i in movable]), spare
        for i in movable:
            extra = min(reach - counts[i], max(1, left * weights[i] // pool), spare)
            counts[i] = counts[i] + extra
            spare = spare - extra
    return np.array(counts)


def bell_draw(stream_key, dims, width, limit, split=(), kind=jnp.bfloat16):
    entries = jax.random.normal(stream_key, dims, jnp.float32) * width
    if len(split) > 0:
        entries = levels(stream_key, dims, split, -0.22, 0.18) * entries
    return jnp.clip(entries, min=-limit, max=limit).astype(kind)


def gaussian_with(rng, dims, scale, limit, pieces, heavy, kind=jnp.bfloat16):
    drawn = scale * jax.random.normal(rng, dims, jnp.float32)
    if pieces:
        drawn = drawn * levels(rng, dims, pieces, -0.22, 0.18)
    return jnp.clip(strengthened(drawn, jax.random.fold_in(rng, 3), *heavy), -limit, limit).astype(kind)


def setup_inputs(seed: int = 0) -> dict:
    streams_of = jax.random.split(jax.random.key(seed), 24)
    tokens = bell_draw(streams_of[0], (B_TOT, D), 1.0, 6.0, ((0, 8),))
    recurrent_head_state = bell_draw(streams_of[1], (B_TOT, HEAD_COUNT, HEAD_WIDTH * HEAD_WIDTH), 0.5, 4.0, ((0, 8), (1, 4)), jnp.float32)
    first_norm_gain = jnp.clip(1.0 + 0.18 * jax.random.normal(streams_of[2], (D,), jnp.float32), 0.1, 1.9)
    receptance_matrix = bell_draw(streams_of[3], (D, HEAD_COUNT * HEAD_WIDTH), D ** -0.5, 0.125, ((1, 4),))
    key_matrix = bell_draw(streams_of[4], (D, HEAD_COUNT * HEAD_WIDTH), D ** -0.5, 0.125, ((1, 4),))
    value_matrix = bell_draw(streams_of[5], (D, HEAD_COUNT * HEAD_WIDTH), D ** -0.5, 0.125, ((1, 4),))
    decay_matrix = bell_draw(streams_of[6], (D, HEAD_COUNT * HEAD_WIDTH), D ** -0.5, 0.125, ((1, 4),))
    decay_offset = jnp.clip(-3.0 + 3.5 * jax.random.uniform(streams_of[7], (HEAD_COUNT * HEAD_WIDTH,), jnp.float32) ** levels(streams_of[7], (HEAD_COUNT * HEAD_WIDTH,), ((0, 4),), -0.2, 0.2), -3.0, 0.5)
    correction_offset = jnp.clip(jax.random.uniform(streams_of[8], (HEAD_COUNT * HEAD_WIDTH,), jnp.float32, -2.0, 2.0) * levels(streams_of[8], (HEAD_COUNT * HEAD_WIDTH,), ((0, 4),), -0.4, 0.0), -2.0, 2.0)
    correction_key_factor = jnp.clip(jax.random.uniform(streams_of[9], (HEAD_COUNT * HEAD_WIDTH,), jnp.float32, -1.0, 1.0) * levels(streams_of[9], (HEAD_COUNT * HEAD_WIDTH,), ((0, 4),), -0.4, 0.0), -1.0, 1.0)
    own_term_weight = bell_draw(streams_of[10], (HEAD_COUNT * HEAD_WIDTH,), 0.15, 0.9, ((0, 4),), jnp.float32)
    head_norm_gain = jnp.clip(1.0 + 0.18 * jax.random.normal(streams_of[11], (HEAD_COUNT * HEAD_WIDTH,), jnp.float32), 0.1, 1.9)
    output_matrix = bell_draw(streams_of[12], (HEAD_COUNT * HEAD_WIDTH, D), (HEAD_COUNT * HEAD_WIDTH) ** -0.5, 0.1875, ((0, 4),))
    second_norm_gain = jnp.clip(1.0 + 0.18 * jax.random.normal(streams_of[13], (D,), jnp.float32), 0.1, 1.9)
    routing_keys = jax.random.split(jax.random.fold_in(streams_of[14], 1), B_TOT // B_DEV)
    routing_turns = jax.random.permutation(jax.random.fold_in(streams_of[14], 3), B_TOT // B_DEV)
    routing = jax.vmap(lambda own, number: shared_out(jax.random.fold_in(streams_of[14], 2), own, number, B_DEV, EXPERTS, TOP_K, CAP, 2))(routing_keys, routing_turns).reshape((B_TOT, TOP_K))
    routing_weight = jnp.clip(0.1 + 0.9 * jax.random.uniform(streams_of[15], (B_TOT, TOP_K), jnp.float32) ** levels(streams_of[15], (B_TOT, TOP_K), ((0, 8),), -0.2, 0.2), 0.1, 1.0)
    expert_gate_weight = bell_draw(streams_of[16], (EXPERTS, D, FF_E), D ** -0.5, 0.125, ((0, 8), (2, 4)))
    expert_up_weight = bell_draw(streams_of[17], (EXPERTS, D, FF_E), D ** -0.5, 0.125, ((0, 8), (2, 4)))
    expert_down_weight = gaussian_with(streams_of[18], (EXPERTS, FF_E, D), FF_E ** -0.5, 0.125, ((0, 8), (1, 4)), (1, 2, 4, 2.0))
    dense_gate_weight = bell_draw(streams_of[19], (D, FF_D), D ** -0.5, 0.125, ((1, 8),))
    dense_up_weight = bell_draw(streams_of[20], (D, FF_D), D ** -0.5, 0.125, ((1, 8),))
    dense_down_weight = bell_draw(streams_of[21], (FF_D, D), FF_D ** -0.5, 0.109375, ((0, 8),))
    dense_gate_offset = jnp.clip(jax.random.uniform(streams_of[22], (D,), jnp.float32, -3.0, 3.0), -3.0, 3.0)
    return {"tokens": tokens, "recurrent_head_state": recurrent_head_state, "first_norm_gain": first_norm_gain, "receptance_matrix": receptance_matrix, "key_matrix": key_matrix, "value_matrix": value_matrix, "decay_matrix": decay_matrix, "decay_offset": decay_offset, "correction_offset": correction_offset, "correction_key_factor": correction_key_factor, "own_term_weight": own_term_weight, "head_norm_gain": head_norm_gain, "output_matrix": output_matrix, "second_norm_gain": second_norm_gain, "routing": routing, "routing_weight": routing_weight, "expert_gate_weight": expert_gate_weight, "expert_up_weight": expert_up_weight, "expert_down_weight": expert_down_weight, "dense_gate_weight": dense_gate_weight, "dense_up_weight": dense_up_weight, "dense_down_weight": dense_down_weight, "dense_gate_offset": dense_gate_offset}


PRECISE = lax.Precision.HIGHEST

def rms_scale(rows, gain):
    floats = rows.astype(jnp.float32)
    return floats * lax.rsqrt(lax.optimization_barrier(jnp.mean(floats * floats, axis=-1, keepdims=True)) + 1e-06) * gain

def route_table(block_routes, experts, capacity):
    flat_routes = block_routes.reshape(-1)
    chosen = (flat_routes[:, None] == jnp.arange(experts, dtype=jnp.int32)[None, :]).astype(jnp.int32)
    before = jnp.cumsum(chosen, axis=0, dtype=jnp.int32) - chosen
    slot_index = lax.optimization_barrier(jnp.sum(before * chosen, axis=1))
    slot_match = (slot_index[:, None] == jnp.arange(capacity, dtype=jnp.int32)[None, :]).astype(jnp.float32)
    dispatch_table = chosen.astype(jnp.float32)[:, :, None] * slot_match[:, None, :]
    return dispatch_table.reshape(block_routes.shape[0], block_routes.shape[1], experts, capacity)

def state_update(receptance_rows, key_matrix_rows, value_matrix_rows, decay_logits, recurrent_head_state, decay_offset, correction_offset, correction_key_factor, own_term_weight, head_norm_gain, head_width):
    seq_count = key_matrix_rows.shape[0]
    decay_factor = jnp.exp(-jnp.exp(decay_offset + decay_logits))
    in_rate = jax.nn.sigmoid(correction_offset + correction_key_factor * key_matrix_rows)
    key_in = key_matrix_rows * in_rate

    def split_heads(block):
        return block.reshape(seq_count, -1, head_width)
    keys_head = split_heads(key_matrix_rows)
    unit_keys = keys_head * lax.rsqrt(lax.optimization_barrier(jnp.mean(keys_head * keys_head, axis=-1, keepdims=True)) + 1e-06) * head_width ** (-0.5)
    rate_head = split_heads(in_rate)
    head_keys = split_heads(key_in)
    decay_head = split_heads(decay_factor)
    head_values = split_heads(value_matrix_rows)
    head_receptance = split_heads(receptance_rows)
    matrix = recurrent_head_state.reshape(seq_count, -1, head_width, head_width)
    removed = jnp.einsum('bhvk,bhk->bhv', matrix, unit_keys, precision=PRECISE)
    updated = matrix * decay_head[:, :, None, :] - removed[..., None] * (unit_keys * rate_head)[:, :, None, :] + head_values[..., None] * head_keys[:, :, None, :]
    readout = jnp.einsum('bhvk,bhk->bhv', updated, head_receptance, precision=PRECISE)
    center = lax.optimization_barrier(jnp.mean(readout, axis=-1, keepdims=True))
    spread = lax.optimization_barrier(jnp.mean(jnp.square(readout - center), axis=-1, keepdims=True))
    normalized_rows = (readout - center) * lax.rsqrt(spread + 0.00064) * head_norm_gain.reshape(-1, head_width)
    own_term_total = lax.optimization_barrier(jnp.sum(head_receptance * head_keys * own_term_weight.reshape(-1, head_width), axis=-1, keepdims=True))
    normalized_rows = normalized_rows + own_term_total * head_values
    return (normalized_rows.reshape(seq_count, -1).astype(jnp.bfloat16), updated.reshape(seq_count, -1, head_width * head_width))

def reference(tokens, recurrent_head_state, first_norm_gain, receptance_matrix, key_matrix, value_matrix, decay_matrix, decay_offset, correction_offset, correction_key_factor, own_term_weight, head_norm_gain, output_matrix, second_norm_gain, routing, routing_weight, expert_gate_weight, expert_up_weight, expert_down_weight, dense_gate_weight, dense_up_weight, dense_down_weight, dense_gate_offset):
    normalized_rows = rms_scale(tokens, first_norm_gain).astype(jnp.bfloat16)
    receptance_rows = jnp.dot(normalized_rows, receptance_matrix, preferred_element_type=jnp.float32)
    key_matrix_rows = jnp.dot(normalized_rows, key_matrix, preferred_element_type=jnp.float32)
    value_matrix_rows = jnp.dot(normalized_rows, value_matrix, preferred_element_type=jnp.float32)
    decay_logits = jnp.dot(normalized_rows, decay_matrix, preferred_element_type=jnp.float32)
    head_outputs, next_state = state_update(receptance_rows, key_matrix_rows, value_matrix_rows, decay_logits, recurrent_head_state, decay_offset, correction_offset, correction_key_factor, own_term_weight, head_norm_gain, HEAD_WIDTH)
    hidden_sum = tokens.astype(jnp.float32) + jnp.dot(head_outputs, output_matrix, preferred_element_type=jnp.float32)
    ffn_in = rms_scale(hidden_sum, second_norm_gain).astype(jnp.bfloat16)
    tables = jax.vmap(partial(route_table, experts=EXPERTS, capacity=CAP))(routing.reshape(N_EP, B_DEV, TOP_K))
    grouped = ffn_in.reshape(N_EP, B_DEV, D).astype(jnp.float32)
    buffers = jnp.einsum('sbkec,sbd->escd', tables, grouped, precision=PRECISE).astype(jnp.bfloat16)

    def one_expert(packed):
        rows, gate_part, up_part, down_part = packed
        flat_rows = rows.reshape(-1, D)
        gate_pre = jnp.dot(flat_rows, gate_part, preferred_element_type=jnp.float32)
        up_pre = jnp.dot(flat_rows, up_part, preferred_element_type=jnp.float32)
        hidden = (jax.nn.silu(gate_pre) * up_pre).astype(jnp.bfloat16)
        result = jnp.dot(hidden, down_part, preferred_element_type=jnp.float32).astype(jnp.bfloat16)
        return result.reshape(rows.shape)
    expert_outs = lax.map(one_expert, (buffers, expert_gate_weight, expert_up_weight, expert_down_weight))
    weighted = jnp.einsum('sbkec,sbk->secb', tables, routing_weight.reshape(N_EP, B_DEV, TOP_K), precision=PRECISE)
    moe = jnp.einsum('secb,escd->sbd', weighted, expert_outs.astype(jnp.float32), precision=PRECISE).reshape(B_TOT, D)
    dense_hidden = (jax.nn.silu(jnp.dot(ffn_in, dense_gate_weight, preferred_element_type=jnp.float32)) * jnp.dot(ffn_in, dense_up_weight, preferred_element_type=jnp.float32)).astype(jnp.bfloat16)
    block_units = FF_D // N_EP

    def add_block(total, index):
        start = index * block_units
        piece = lax.dynamic_slice_in_dim(dense_hidden, start, block_units, 1)
        rows = lax.dynamic_slice_in_dim(dense_down_weight, start, block_units, 0)
        part = jnp.dot(piece, rows, preferred_element_type=jnp.float32).astype(jnp.bfloat16)
        part = lax.optimization_barrier(part)
        return (total + part.astype(jnp.float32), None)
    dense_sum, _ = lax.scan(add_block, jnp.zeros((B_TOT, D), jnp.float32), jnp.arange(N_EP, dtype=jnp.int32))
    layer_out = (hidden_sum + moe + jax.nn.sigmoid(dense_gate_offset) * dense_sum).astype(jnp.bfloat16)
    return (layer_out, next_state)
```

```python
import functools

import jax
import jax.numpy as jnp
from jax import lax
from jax.experimental import pallas as pl
from jax.experimental.pallas import tpu as pltpu
from jax.sharding import PartitionSpec as P

HEAD_WIDTH = 64


PRECISE = lax.Precision.HIGHEST


def rms_scale(rows, gain):
    floats = rows.astype(jnp.float32)
    return floats * lax.rsqrt(jnp.mean(floats * floats, axis=-1, keepdims=True) + 1e-06) * gain


def route_table(block_routes, experts, capacity):
    flat_routes = block_routes.reshape(-1)
    chosen = (flat_routes[:, None] == jnp.arange(experts, dtype=jnp.int32)[None, :]).astype(
        jnp.int32
    )
    before = jnp.cumsum(chosen, axis=0, dtype=jnp.int32) - chosen
    slot_index = jnp.sum(before * chosen, axis=1)
    slot_match = (slot_index[:, None] == jnp.arange(capacity, dtype=jnp.int32)[None, :]).astype(
        jnp.float32
    )
    dispatch_table = chosen.astype(jnp.float32)[:, :, None] * slot_match[:, None, :]
    return dispatch_table.reshape(block_routes.shape[0], block_routes.shape[1], experts, capacity)


def state_update(
    receptance_rows,
    key_matrix_rows,
    value_matrix_rows,
    decay_logits,
    recurrent_head_state,
    decay_offset,
    correction_offset,
    correction_key_factor,
    own_term_weight,
    head_norm_gain,
    head_width,
):
    seq_count = key_matrix_rows.shape[0]
    decay_factor = jnp.exp(-jnp.exp(decay_offset + decay_logits))
    in_rate = jax.nn.sigmoid(correction_offset + correction_key_factor * key_matrix_rows)
    key_in = key_matrix_rows * in_rate

    def split_heads(block):
        return block.reshape(seq_count, -1, head_width)

    keys_head = split_heads(key_matrix_rows)
    unit_keys = (
        keys_head
        * lax.rsqrt(jnp.mean(keys_head * keys_head, axis=-1, keepdims=True) + 1e-06)
        * head_width ** (-0.5)
    )
    rate_head = split_heads(in_rate)
    head_keys = split_heads(key_in)
    decay_head = split_heads(decay_factor)
    head_values = split_heads(value_matrix_rows)
    head_receptance = split_heads(receptance_rows)
    matrix = recurrent_head_state.reshape(seq_count, -1, head_width, head_width)
    removed = jnp.einsum("bhvk,bhk->bhv", matrix, unit_keys, precision=PRECISE)
    updated = (
        matrix * decay_head[:, :, None, :]
        - removed[..., None] * (unit_keys * rate_head)[:, :, None, :]
        + head_values[..., None] * head_keys[:, :, None, :]
    )
    readout = jnp.einsum("bhvk,bhk->bhv", updated, head_receptance, precision=PRECISE)
    center = jnp.mean(readout, axis=-1, keepdims=True)
    spread = jnp.mean(jnp.square(readout - center), axis=-1, keepdims=True)
    normalized_rows = (
        (readout - center) * lax.rsqrt(spread + 0.00064) * head_norm_gain.reshape(-1, head_width)
    )
    own_term_total = jnp.sum(
        head_receptance * head_keys * own_term_weight.reshape(-1, head_width),
        axis=-1,
        keepdims=True,
    )
    normalized_rows = normalized_rows + own_term_total * head_values
    return (
        normalized_rows.reshape(seq_count, -1).astype(jnp.bfloat16),
        updated.reshape(seq_count, -1, head_width * head_width),
    )


def local(
    tokens,
    recurrent_head_state,
    first_norm_gain,
    receptance_matrix,
    key_matrix,
    value_matrix,
    decay_matrix,
    decay_offset,
    correction_offset,
    correction_key_factor,
    own_term_weight,
    head_norm_gain,
    output_matrix,
    second_norm_gain,
    routing,
    routing_weight,
    expert_gate_weight,
    expert_up_weight,
    expert_down_weight,
    dense_gate_weight,
    dense_up_weight,
    dense_down_weight,
    dense_gate_offset,
):
    seq_count = tokens.shape[0]
    width = tokens.shape[1]
    group_index = lax.axis_index("ep")
    lane_index = lax.axis_index("tp")
    group_count = lax.axis_size("ep")
    lane_count = lax.axis_size("tp")
    normalized_rows = rms_scale(tokens, first_norm_gain).astype(jnp.bfloat16)
    receptance_rows = jnp.dot(
        normalized_rows, receptance_matrix, preferred_element_type=jnp.float32
    )
    key_matrix_rows = jnp.dot(normalized_rows, key_matrix, preferred_element_type=jnp.float32)
    value_matrix_rows = jnp.dot(normalized_rows, value_matrix, preferred_element_type=jnp.float32)
    decay_logits = jnp.dot(normalized_rows, decay_matrix, preferred_element_type=jnp.float32)
    head_outputs, next_state = state_update(
        receptance_rows,
        key_matrix_rows,
        value_matrix_rows,
        decay_logits,
        recurrent_head_state,
        decay_offset,
        correction_offset,
        correction_key_factor,
        own_term_weight,
        head_norm_gain,
        HEAD_WIDTH,
    )
    partial_out = jnp.dot(head_outputs, output_matrix, preferred_element_type=jnp.float32)
    hidden_sum = tokens.astype(jnp.float32) + lax.psum(
        partial_out.astype(jnp.bfloat16), "tp"
    ).astype(jnp.float32)
    ffn_in = rms_scale(hidden_sum, second_norm_gain).astype(jnp.bfloat16)
    local_experts = expert_gate_weight.shape[0]
    top_count = routing.shape[1]
    expert_count = local_experts * group_count
    capacity = 2 * seq_count * top_count // expert_count
    per_lane = seq_count // lane_count
    own_routes = lax.dynamic_slice_in_dim(routing, group_index * seq_count, seq_count, 0)
    own_table = route_table(own_routes, expert_count, capacity)
    send_rows = jnp.einsum(
        "bkec,bd->ecd", own_table.astype(jnp.bfloat16), ffn_in, preferred_element_type=jnp.float32
    ).astype(jnp.bfloat16)
    lane_rows = lax.dynamic_slice_in_dim(ffn_in, lane_index * per_lane, per_lane, 0)
    dense_send = jnp.broadcast_to(lane_rows[None], (group_count, per_lane, width))
    expert_in, dense_in = (
        lax.all_to_all(send_rows, "ep", split_axis=0, concat_axis=0, tiled=True),
        lax.all_to_all(dense_send, "ep", split_axis=0, concat_axis=0, tiled=True),
    )
    rows_in = expert_in.reshape(group_count, local_experts, capacity, width).transpose(1, 0, 2, 3)
    rows_in = rows_in.reshape(local_experts, group_count * capacity, width)
    gate_pre = jnp.einsum(
        "lrd,ldf->lrf", rows_in, expert_gate_weight, preferred_element_type=jnp.float32
    )
    up_pre = jnp.einsum(
        "lrd,ldf->lrf", rows_in, expert_up_weight, preferred_element_type=jnp.float32
    )
    expert_hidden = (jax.nn.silu(gate_pre) * up_pre).astype(jnp.bfloat16)
    expert_part = jnp.einsum(
        "lrf,lfd->lrd", expert_hidden, expert_down_weight, preferred_element_type=jnp.float32
    )
    expert_out = lax.psum_scatter(
        expert_part.astype(jnp.bfloat16), "tp", scatter_dimension=2, tiled=True
    )
    back_send = expert_out.reshape(local_experts, group_count, capacity, -1).transpose(1, 0, 2, 3)
    back_send = back_send.reshape(group_count * local_experts, capacity, -1)
    dense_rows = dense_in.reshape(group_count * per_lane, width)
    dense_hidden = (
        jax.nn.silu(jnp.dot(dense_rows, dense_gate_weight, preferred_element_type=jnp.float32))
        * jnp.dot(dense_rows, dense_up_weight, preferred_element_type=jnp.float32)
    ).astype(jnp.bfloat16)
    dense_part = jnp.dot(
        dense_hidden, dense_down_weight, preferred_element_type=jnp.float32
    ).astype(jnp.bfloat16)
    dense_part = dense_part.reshape(group_count, per_lane, width)
    back_experts, back_dense = (
        lax.all_to_all(back_send, "ep", split_axis=0, concat_axis=0, tiled=True),
        lax.all_to_all(dense_part, "ep", split_axis=0, concat_axis=0, tiled=True),
    )
    dense_sum = jnp.sum(back_dense.astype(jnp.float32), axis=0)
    weighted = jnp.einsum("bkec,bk->ecb", own_table, routing_weight, precision=PRECISE)
    moe_slice = jnp.einsum(
        "ecb,ecd->bd", weighted, back_experts.astype(jnp.float32), precision=PRECISE
    )
    moe_rows = lax.all_to_all(moe_slice, "tp", split_axis=0, concat_axis=1, tiled=True)
    residual_rows = lax.dynamic_slice_in_dim(hidden_sum, lane_index * per_lane, per_lane, 0)
    layer_out = (residual_rows + moe_rows + jax.nn.sigmoid(dense_gate_offset) * dense_sum).astype(
        jnp.bfloat16
    )
    return (layer_out, next_state)


def proj_state_kernel(
    tokens_ref, gain_ref, wr_ref, wk_ref, wv_ref, wd_ref, doff_ref, coff_ref, cfac_ref,
    own_ref, hgain_ref, wo_ref, routes_ref, rweight_ref, state_ref,
    next_ref, part_ref, base_ref, wext_ref,
    sbuf, nbuf, in_sem, out_sem,
):
    seqs, width = tokens_ref.shape
    heads = state_ref.shape[1]
    lanes = part_ref.shape[0]
    rows = part_ref.shape[1]
    loads = [
        pltpu.make_async_copy(state_ref.at[:, h, :], sbuf.at[h], in_sem.at[h]) for h in range(heads)
    ]
    for load in loads:
        load.start()
    f32, bf16 = jnp.float32, jnp.bfloat16
    toks = tokens_ref[...].astype(f32)
    normed = (
        toks * lax.rsqrt(jnp.mean(toks * toks, axis=-1, keepdims=True) + 1e-06) * gain_ref[...]
    ).astype(bf16)
    recept = jnp.dot(normed, wr_ref[...], preferred_element_type=f32)
    keys = jnp.dot(normed, wk_ref[...], preferred_element_type=f32)
    values = jnp.dot(normed, wv_ref[...], preferred_element_type=f32)
    logits = jnp.dot(normed, wd_ref[...], preferred_element_type=f32)
    decay = jnp.exp(-jnp.exp(doff_ref[...] + logits))
    rate = jax.nn.sigmoid(coff_ref[...] + cfac_ref[...] * keys)
    key_in = keys * rate
    own_prod = recept * key_in * own_ref[...]
    hgain = jnp.broadcast_to(hgain_ref[...], keys.shape)
    pair = 2 * HEAD_WIDTH
    lane = lax.broadcasted_iota(jnp.int32, (seqs, pair), 1)
    low = lane < HEAD_WIDTH
    half_r = lax.broadcasted_iota(jnp.int32, (pair, pair), 0) // HEAD_WIDTH
    half_c = lax.broadcasted_iota(jnp.int32, (pair, pair), 1) // HEAD_WIDTH
    ones_block = (half_r == half_c).astype(f32).astype(bf16)

    def group_sum(block):
        high = block.astype(bf16)
        rest = (block - high.astype(f32)).astype(bf16)
        return jnp.dot(high, ones_block, preferred_element_type=f32) + jnp.dot(
            rest, ones_block, preferred_element_type=f32
        )

    def doubled(full, h):
        chunk = full[:, (h // 2) * pair : (h // 2 + 1) * pair]
        turned = pltpu.roll(chunk, HEAD_WIDTH, 1)
        return jnp.where(low, chunk, turned) if h % 2 == 0 else jnp.where(low, turned, chunk)

    chunks = state_ref.shape[2] // pair
    step = 8
    outs, stores = [], []
    for h in range(heads):
        k2, r2, v2 = doubled(keys, h), doubled(recept, h), doubled(values, h)
        d2, kin2, rate2 = doubled(decay, h), doubled(key_in, h), doubled(rate, h)
        unit = (
            k2
            * lax.rsqrt(jnp.mean(k2 * k2, axis=-1, keepdims=True) + 1e-06)
            * HEAD_WIDTH ** (-0.5)
        )
        own_total = 0.5 * jnp.sum(doubled(own_prod, h), axis=-1, keepdims=True)

        def many(block):
            return jnp.concatenate([block] * step, axis=0)

        unit_m, back_m, dec_m = many(unit), many(unit * rate2), many(d2)
        kin_m, rec_m = many(kin2), many(r2)
        loads[h].wait()
        acc = jnp.zeros((seqs, pair), f32)
        for q in range(0, chunks, step):
            picks = [(lane == 2 * j) | (lane == HEAD_WIDTH + 2 * j + 1) for j in range(q, q + step)]
            old = jnp.concatenate(
                [sbuf[h, :, j * pair : (j + 1) * pair] for j in range(q, q + step)], axis=0
            )
            removed = group_sum(old * unit_m)
            spread_v = group_sum(jnp.concatenate([jnp.where(p, v2, 0.0) for p in picks], axis=0))
            new = old * dec_m - removed * back_m + spread_v * kin_m
            for i in range(step):
                nbuf[h, :, (q + i) * pair : (q + i + 1) * pair] = new[i * seqs : (i + 1) * seqs]
            read = group_sum(new * rec_m)
            for i in range(step):
                acc = acc + jnp.where(picks[i], read[i * seqs : (i + 1) * seqs], 0.0)
        store = pltpu.make_async_copy(nbuf.at[h], next_ref.at[:, h, :], out_sem.at[h])
        store.start()
        stores.append(store)
        y = acc + pltpu.roll(acc, HEAD_WIDTH, 1)
        center = y - jnp.mean(y, axis=-1, keepdims=True)
        var = jnp.mean(center * center, axis=-1, keepdims=True)
        outs.append(center * lax.rsqrt(var + 0.00064) * doubled(hgain, h) + own_total * v2)
    merged = jnp.concatenate(
        [jnp.where(low, outs[h], outs[h + 1]) for h in range(0, heads, 2)], axis=1
    ).astype(bf16)
    part = jnp.dot(merged, wo_ref[...], preferred_element_type=f32)
    me_lane = lax.axis_index("tp")
    base = jnp.zeros((rows, width), f32)
    for i in range(lanes):
        mine = part[i * rows : (i + 1) * rows]
        part_ref[i] = mine.astype(bf16)
        base = jnp.where(me_lane == i, mine + toks[i * rows : (i + 1) * rows], base)
    base_ref[...] = base
    start = pl.multiple_of(lax.axis_index("ep") * seqs + me_lane * rows, 8)
    own_start = pl.multiple_of(me_lane * rows, 8)
    routes = routes_ref[pl.ds(start, rows), :]
    weights = rweight_ref[pl.ds(own_start, rows), :]
    column = lax.broadcasted_iota(jnp.int32, (rows, 128), 1) % 64
    table = jnp.zeros((rows, 128), f32)
    for k in range(routes.shape[1]):
        table = table + jnp.where(column == routes[:, k : k + 1], weights[:, k : k + 1], 0.0)
    wext_ref[...] = table
    for store in stores:
        store.wait()


def exchange_kernel(
    groups, lanes,
    part_ref, base_ref, wext_ref, gain_ref, goff_ref,
    eg_hbm, eu_hbm, ed_hbm, dg_hbm, du_hbm, dd_hbm,
    out_ref,
    eg, eu, ed, dg, du, dd, p_in, xs, flat, hid, dens, ys, y_in, z_in, v_out, v_in,
    w_sem, s1, r1, sz, rz, st, rt, sc, rc, sa, ra, sb, rb, sv, rv,
):
    f32, bf16 = jnp.float32, jnp.bfloat16
    rows, width = base_ref.shape
    zs = groups // 2
    me_g, me_l = lax.axis_index("ep"), lax.axis_index("tp")
    core, me_z = lax.rem(me_g, 2), me_g // 2
    partner = (me_g + 1 - 2 * core, me_l)

    def lane_peer(d):
        return (me_g, lax.rem(me_l + d + lanes, lanes))

    def z_peer(d):
        return (lax.rem(me_z + d + zs, zs) * 2 + core, me_l)

    def send(src, dst, ssem, rsem, peer):
        copy = pltpu.make_async_remote_copy(
            src_ref=src, dst_ref=dst, send_sem=ssem, recv_sem=rsem, device_id=peer,
            device_id_type=pl.DeviceIdType.MESH,
        )
        copy.start()
        return copy

    pulls = [
        pltpu.make_async_copy(src, dst, w_sem.at[i])
        for i, (src, dst) in enumerate(
            [(dg_hbm, dg), (du_hbm, du), (dd_hbm, dd), (eg_hbm.at[0], eg), (eu_hbm.at[0], eu),
             (ed_hbm.at[0], ed)]
        )
    ]
    for pull in pulls:
        pull.start()
    barrier = pltpu.get_barrier_semaphore()
    peers = [lane_peer(d) for d in range(1, lanes)] + [z_peer(d) for d in range(1, zs)] + [partner]
    for peer in peers:
        pl.semaphore_signal(barrier, inc=1, device_id=peer, device_id_type=pl.DeviceIdType.MESH)
    pl.semaphore_wait(barrier, len(peers))
    sent = []
    firsts = []
    for d in range(1, lanes):
        target = lax.rem(me_l + lanes - d, lanes)
        firsts.append(
            send(part_ref.at[target], p_in.at[d - 1], s1.at[d - 1], r1.at[d - 1], (me_g, target))
        )
    hidden = base_ref[...]
    for d, copy in enumerate(firsts):
        copy.wait_recv()
        hidden = hidden + p_in[d].astype(f32)
    sent += firsts
    normed = hidden * lax.rsqrt(jnp.mean(hidden * hidden, axis=-1, keepdims=True) + 1e-06)
    xs[0, 0, 0, :, :width] = (normed * gain_ref[...]).astype(bf16)
    table = wext_ref[...]
    high = table.astype(bf16).astype(f32)
    first_half = lax.broadcasted_iota(jnp.int32, table.shape, 1) < 64
    xs[0, 0, 0, :, width:] = jnp.where(first_half, high, table - high).astype(bf16)
    hold_z, hold_t, hold_c = {}, {}, {}
    for d in range(1, zs):
        hold_z[d] = send(xs.at[0, 0, 0], xs.at[0, 0, d], sz.at[d - 1], rz.at[d - 1], z_peer(d))

    def to_partner(d, q):
        i = d * zs + q
        hold_c[d, q] = send(xs.at[0, d, q], xs.at[1, d, q], sc.at[i], rc.at[i], partner)

    def to_lanes(q):
        to_partner(0, q)
        for d in range(1, lanes):
            i = (d - 1) * zs + q
            hold_t[d, q] = send(xs.at[0, 0, q], xs.at[0, d, q], st.at[i], rt.at[i], lane_peer(d))

    to_lanes(0)
    for q in range(1, zs):
        hold_z[q].wait_recv()
        to_lanes(q)
    block = 2 * zs * rows

    def gathered(d):
        return xs[:, d].astype(f32).reshape(block, width + 128)

    for q in range(zs):
        hold_c[0, q].wait_recv()
    mine = gathered(0)
    flat[0:block] = mine.astype(bf16)
    own_rows = mine[:, :width].astype(bf16)
    for pull in pulls[:3]:
        pull.wait()
    gate = jnp.dot(own_rows, dg[...], preferred_element_type=f32)
    up = jnp.dot(own_rows, du[...], preferred_element_type=f32)
    mixed = (jax.nn.silu(gate) * up).astype(bf16)
    dens[...] = jnp.dot(mixed, dd[...], preferred_element_type=f32) * jax.nn.sigmoid(goff_ref[...])
    for q in range(zs):
        for d in range(1, lanes):
            hold_t[d, q].wait_recv()
            to_partner(d, q)
    for d in range(1, lanes):
        for q in range(zs):
            hold_c[d, q].wait_recv()
        flat[d * block : (d + 1) * block] = gathered(d).astype(bf16)
    for pull in pulls[3:]:
        pull.wait()
    tile = 256

    @pl.loop(0, eg.shape[1] // tile)
    def _(n):
        cols = pl.ds(pl.multiple_of(n * tile, tile), tile)
        left = flat[:, :width]
        gated = jnp.dot(left, eg[:, cols], preferred_element_type=f32)
        raised = jnp.dot(left, eu[:, cols], preferred_element_type=f32)
        hid[:, cols] = (jax.nn.silu(gated) * raised).astype(bf16)

    tail = flat[:, width:].astype(f32)
    picked = lax.broadcasted_iota(jnp.int32, tail.shape, 1) % 64 == me_g
    scale = jnp.sum(jnp.where(picked, tail, 0.0), axis=-1, keepdims=True)
    wide = 256

    @pl.loop(0, width // wide)
    def _(n):
        cols = pl.ds(pl.multiple_of(n * wide, wide), wide)
        made = jnp.dot(hid[...], ed[:, cols], preferred_element_type=f32) * scale
        for d in range(lanes):
            piece = made[d * block : (d + 1) * block]
            if d == 0:
                piece = piece + dens[:, cols]
            ys[:, d, :, :, cols] = piece.reshape(2, zs, rows, wide).astype(bf16)

    to_core = [
        send(ys.at[1, d], y_in.at[d], sa.at[d], ra.at[d], partner)
        for d in list(range(1, lanes)) + [0]
    ]
    to_lane = []
    for d in range(1, lanes):
        to_core[d - 1].wait_recv()
        ys[0, d] = (ys[0, d].astype(f32) + y_in[d].astype(f32)).astype(bf16)
        to_lane.append(
            send(ys.at[0, d], z_in.at[d - 1], sb.at[d - 1], rb.at[d - 1], lane_peer(-d))
        )
    to_core[lanes - 1].wait_recv()
    total = ys[0, 0].astype(f32) + y_in[0].astype(f32)
    for d in range(1, lanes):
        to_lane[d - 1].wait_recv()
        total = total + z_in[d - 1].astype(f32)
    v_out[...] = total.astype(bf16)
    to_z = [
        send(v_out.at[d], v_in.at[d - 1], sv.at[d - 1], rv.at[d - 1], z_peer(-d))
        for d in range(1, zs)
    ]
    result = hidden + total[0]
    for d, copy in enumerate(to_z):
        copy.wait_recv()
        result = result + v_in[d].astype(f32)
    out_ref[...] = result.astype(bf16)
    sent += list(hold_z.values()) + list(hold_t.values()) + list(hold_c.values())
    sent += to_core + to_lane + to_z
    for copy in sent:
        copy.wait_send()


def fused(
    tokens, recurrent_head_state, first_norm_gain, receptance_matrix, key_matrix, value_matrix,
    decay_matrix, decay_offset, correction_offset, correction_key_factor, own_term_weight,
    head_norm_gain, output_matrix, second_norm_gain, routing, routing_weight, expert_gate_weight,
    expert_up_weight, expert_down_weight, dense_gate_weight, dense_up_weight, dense_down_weight,
    dense_gate_offset,
):
    f32, bf16 = jnp.float32, jnp.bfloat16
    seqs, width = tokens.shape
    heads, flat_width = recurrent_head_state.shape[1:]
    groups, lanes = lax.axis_size("ep"), lax.axis_size("tp")
    rows, zs = seqs // lanes, groups // 2
    vmem = pl.BlockSpec(memory_space=pltpu.VMEM)
    anywhere = pl.BlockSpec(memory_space=pl.ANY)
    dma = pltpu.SemaphoreType.DMA

    def row(vector):
        return vector.reshape(1, -1)

    next_state, part, base, table = pl.pallas_call(
        proj_state_kernel,
        out_shape=(
            jax.ShapeDtypeStruct(recurrent_head_state.shape, f32),
            jax.ShapeDtypeStruct((lanes, rows, width), bf16),
            jax.ShapeDtypeStruct((rows, width), f32),
            jax.ShapeDtypeStruct((rows, 128), f32),
        ),
        in_specs=[vmem] * 14 + [anywhere],
        out_specs=(anywhere, vmem, vmem, vmem),
        scratch_shapes=[
            pltpu.VMEM((heads, seqs, flat_width), f32),
            pltpu.VMEM((heads, seqs, flat_width), f32),
            dma((heads,)),
            dma((heads,)),
        ],
        compiler_params=pltpu.CompilerParams(vmem_limit_bytes=40 * 1024 * 1024),
        name="proj_state",
    )(
        tokens, row(first_norm_gain), receptance_matrix, key_matrix, value_matrix, decay_matrix,
        row(decay_offset), row(correction_offset), row(correction_key_factor),
        row(own_term_weight), row(head_norm_gain), output_matrix, routing, routing_weight,
        recurrent_head_state,
    )
    hidden_units = expert_gate_weight.shape[2]
    total = groups * seqs
    layer_out = pl.pallas_call(
        functools.partial(exchange_kernel, groups, lanes),
        out_shape=jax.ShapeDtypeStruct((rows, width), bf16),
        in_specs=[vmem] * 5 + [anywhere] * 6,
        out_specs=vmem,
        scratch_shapes=[
            pltpu.VMEM(expert_gate_weight.shape[1:], bf16),
            pltpu.VMEM(expert_up_weight.shape[1:], bf16),
            pltpu.VMEM(expert_down_weight.shape[1:], bf16),
            pltpu.VMEM(dense_gate_weight.shape, bf16),
            pltpu.VMEM(dense_up_weight.shape, bf16),
            pltpu.VMEM(dense_down_weight.shape, bf16),
            pltpu.VMEM((lanes - 1, rows, width), bf16),
            pltpu.VMEM((2, lanes, zs, rows, width + 128), bf16),
            pltpu.VMEM((total, width + 128), bf16),
            pltpu.VMEM((total, hidden_units), bf16),
            pltpu.VMEM((2 * zs * rows, width), f32),
            pltpu.VMEM((2, lanes, zs, rows, width), bf16),
            pltpu.VMEM((lanes, zs, rows, width), bf16),
            pltpu.VMEM((lanes - 1, zs, rows, width), bf16),
            pltpu.VMEM((zs, rows, width), bf16),
            pltpu.VMEM((zs - 1, rows, width), bf16),
            dma((6,)),
            dma((lanes - 1,)), dma((lanes - 1,)),
            dma((zs - 1,)), dma((zs - 1,)),
            dma(((lanes - 1) * zs,)), dma(((lanes - 1) * zs,)),
            dma((lanes * zs,)), dma((lanes * zs,)),
            dma((lanes,)), dma((lanes,)),
            dma((lanes - 1,)), dma((lanes - 1,)),
            dma((zs - 1,)), dma((zs - 1,)),
        ],
        compiler_params=pltpu.CompilerParams(
            collective_id=0, has_side_effects=True, vmem_limit_bytes=48 * 1024 * 1024
        ),
        name="exchange",
    )(
        part, base, table, row(second_norm_gain), row(dense_gate_offset), expert_gate_weight,
        expert_up_weight, expert_down_weight, dense_gate_weight, dense_up_weight,
        dense_down_weight,
    )
    return (layer_out, next_state)


def choose(tokens, recurrent_head_state, *rest):
    groups, lanes = lax.axis_size("ep"), lax.axis_size("tp")
    rows, heads = tokens.shape[0] // lanes, recurrent_head_state.shape[1]
    experts_here = rest[14].shape[0]
    fits = (
        rows % 8 == 0 and heads % 2 == 0 and groups % 2 == 0 and groups > 2 and lanes > 1
        and groups <= 64 and experts_here == 1
    )
    return (fused if fits else local)(tokens, recurrent_head_state, *rest)


def solution(mesh):
    return jax.shard_map(
        choose,
        mesh=mesh,
        in_specs=(
            P("ep", None),
            P("ep", "tp", None),
            P(),
            P(None, "tp"),
            P(None, "tp"),
            P(None, "tp"),
            P(None, "tp"),
            P("tp"),
            P("tp"),
            P("tp"),
            P("tp"),
            P("tp"),
            P("tp", None),
            P(),
            P(),
            P("ep", None),
            P("ep", None, "tp"),
            P("ep", None, "tp"),
            P("ep", "tp", None),
            P(None, "ep"),
            P(None, "ep"),
            P("ep", None),
            P(),
        ),
        out_specs=(P(("ep", "tp"), None), P("ep", "tp", None)),
        check_vma=False,
    )
```

```python
import functools

import jax
import jax.numpy as jnp
from jax import lax
from jax.experimental import pallas as pl
from jax.experimental.pallas import tpu as pltpu
from jax.sharding import PartitionSpec as P

HEAD_WIDTH = 64
VMEM_BYTES = 67043328


PRECISE = lax.Precision.HIGHEST


def rms_scale(rows, gain):
    floats = rows.astype(jnp.float32)
    return floats * lax.rsqrt(jnp.mean(floats * floats, axis=-1, keepdims=True) + 1e-06) * gain


def route_table(block_routes, experts, capacity):
    flat_routes = block_routes.reshape(-1)
    chosen = (flat_routes[:, None] == jnp.arange(experts, dtype=jnp.int32)[None, :]).astype(
        jnp.int32
    )
    before = jnp.cumsum(chosen, axis=0, dtype=jnp.int32) - chosen
    slot_index = jnp.sum(before * chosen, axis=1)
    slot_match = (slot_index[:, None] == jnp.arange(capacity, dtype=jnp.int32)[None, :]).astype(
        jnp.float32
    )
    dispatch_table = chosen.astype(jnp.float32)[:, :, None] * slot_match[:, None, :]
    return dispatch_table.reshape(block_routes.shape[0], block_routes.shape[1], experts, capacity)


def state_update(
    receptance_rows,
    key_matrix_rows,
    value_matrix_rows,
    decay_logits,
    recurrent_head_state,
    decay_offset,
    correction_offset,
    correction_key_factor,
    own_term_weight,
    head_norm_gain,
    head_width,
):
    seq_count = key_matrix_rows.shape[0]
    decay_factor = jnp.exp(-jnp.exp(decay_offset + decay_logits))
    in_rate = jax.nn.sigmoid(correction_offset + correction_key_factor * key_matrix_rows)
    key_in = key_matrix_rows * in_rate

    def split_heads(block):
        return block.reshape(seq_count, -1, head_width)

    keys_head = split_heads(key_matrix_rows)
    unit_keys = (
        keys_head
        * lax.rsqrt(jnp.mean(keys_head * keys_head, axis=-1, keepdims=True) + 1e-06)
        * head_width ** (-0.5)
    )
    rate_head = split_heads(in_rate)
    head_keys = split_heads(key_in)
    decay_head = split_heads(decay_factor)
    head_values = split_heads(value_matrix_rows)
    head_receptance = split_heads(receptance_rows)
    matrix = recurrent_head_state.reshape(seq_count, -1, head_width, head_width)
    removed = jnp.einsum("bhvk,bhk->bhv", matrix, unit_keys, precision=PRECISE)
    updated = (
        matrix * decay_head[:, :, None, :]
        - removed[..., None] * (unit_keys * rate_head)[:, :, None, :]
        + head_values[..., None] * head_keys[:, :, None, :]
    )
    readout = jnp.einsum("bhvk,bhk->bhv", updated, head_receptance, precision=PRECISE)
    center = jnp.mean(readout, axis=-1, keepdims=True)
    spread = jnp.mean(jnp.square(readout - center), axis=-1, keepdims=True)
    normalized_rows = (
        (readout - center) * lax.rsqrt(spread + 0.00064) * head_norm_gain.reshape(-1, head_width)
    )
    own_term_total = jnp.sum(
        head_receptance * head_keys * own_term_weight.reshape(-1, head_width),
        axis=-1,
        keepdims=True,
    )
    normalized_rows = normalized_rows + own_term_total * head_values
    return (
        normalized_rows.reshape(seq_count, -1).astype(jnp.bfloat16),
        updated.reshape(seq_count, -1, head_width * head_width),
    )


def local(
    tokens,
    recurrent_head_state,
    first_norm_gain,
    receptance_matrix,
    key_matrix,
    value_matrix,
    decay_matrix,
    decay_offset,
    correction_offset,
    correction_key_factor,
    own_term_weight,
    head_norm_gain,
    output_matrix,
    second_norm_gain,
    routing,
    routing_weight,
    expert_gate_weight,
    expert_up_weight,
    expert_down_weight,
    dense_gate_weight,
    dense_up_weight,
    dense_down_weight,
    dense_gate_offset,
):
    seq_count = tokens.shape[0]
    width = tokens.shape[1]
    group_index = lax.axis_index("ep")
    lane_index = lax.axis_index("tp")
    group_count = lax.axis_size("ep")
    lane_count = lax.axis_size("tp")
    normalized_rows = rms_scale(tokens, first_norm_gain).astype(jnp.bfloat16)
    receptance_rows = jnp.dot(
        normalized_rows, receptance_matrix, preferred_element_type=jnp.float32
    )
    key_matrix_rows = jnp.dot(normalized_rows, key_matrix, preferred_element_type=jnp.float32)
    value_matrix_rows = jnp.dot(normalized_rows, value_matrix, preferred_element_type=jnp.float32)
    decay_logits = jnp.dot(normalized_rows, decay_matrix, preferred_element_type=jnp.float32)
    head_outputs, next_state = state_update(
        receptance_rows,
        key_matrix_rows,
        value_matrix_rows,
        decay_logits,
        recurrent_head_state,
        decay_offset,
        correction_offset,
        correction_key_factor,
        own_term_weight,
        head_norm_gain,
        HEAD_WIDTH,
    )
    partial_out = jnp.dot(head_outputs, output_matrix, preferred_element_type=jnp.float32)
    hidden_sum = tokens.astype(jnp.float32) + lax.psum(
        partial_out.astype(jnp.bfloat16), "tp"
    ).astype(jnp.float32)
    ffn_in = rms_scale(hidden_sum, second_norm_gain).astype(jnp.bfloat16)
    local_experts = expert_gate_weight.shape[0]
    top_count = routing.shape[1]
    expert_count = local_experts * group_count
    capacity = 2 * seq_count * top_count // expert_count
    per_lane = seq_count // lane_count
    own_routes = lax.dynamic_slice_in_dim(routing, group_index * seq_count, seq_count, 0)
    own_table = route_table(own_routes, expert_count, capacity)
    send_rows = jnp.einsum(
        "bkec,bd->ecd", own_table.astype(jnp.bfloat16), ffn_in, preferred_element_type=jnp.float32
    ).astype(jnp.bfloat16)
    lane_rows = lax.dynamic_slice_in_dim(ffn_in, lane_index * per_lane, per_lane, 0)
    dense_send = jnp.broadcast_to(lane_rows[None], (group_count, per_lane, width))
    expert_in, dense_in = (
        lax.all_to_all(send_rows, "ep", split_axis=0, concat_axis=0, tiled=True),
        lax.all_to_all(dense_send, "ep", split_axis=0, concat_axis=0, tiled=True),
    )
    rows_in = expert_in.reshape(group_count, local_experts, capacity, width).transpose(1, 0, 2, 3)
    rows_in = rows_in.reshape(local_experts, group_count * capacity, width)
    gate_pre = jnp.einsum(
        "lrd,ldf->lrf", rows_in, expert_gate_weight, preferred_element_type=jnp.float32
    )
    up_pre = jnp.einsum(
        "lrd,ldf->lrf", rows_in, expert_up_weight, preferred_element_type=jnp.float32
    )
    expert_hidden = (jax.nn.silu(gate_pre) * up_pre).astype(jnp.bfloat16)
    expert_part = jnp.einsum(
        "lrf,lfd->lrd", expert_hidden, expert_down_weight, preferred_element_type=jnp.float32
    )
    expert_out = lax.psum_scatter(
        expert_part.astype(jnp.bfloat16), "tp", scatter_dimension=2, tiled=True
    )
    back_send = expert_out.reshape(local_experts, group_count, capacity, -1).transpose(1, 0, 2, 3)
    back_send = back_send.reshape(group_count * local_experts, capacity, -1)
    dense_rows = dense_in.reshape(group_count * per_lane, width)
    dense_hidden = (
        jax.nn.silu(jnp.dot(dense_rows, dense_gate_weight, preferred_element_type=jnp.float32))
        * jnp.dot(dense_rows, dense_up_weight, preferred_element_type=jnp.float32)
    ).astype(jnp.bfloat16)
    dense_part = jnp.dot(
        dense_hidden, dense_down_weight, preferred_element_type=jnp.float32
    ).astype(jnp.bfloat16)
    dense_part = dense_part.reshape(group_count, per_lane, width)
    back_experts, back_dense = (
        lax.all_to_all(back_send, "ep", split_axis=0, concat_axis=0, tiled=True),
        lax.all_to_all(dense_part, "ep", split_axis=0, concat_axis=0, tiled=True),
    )
    dense_sum = jnp.sum(back_dense.astype(jnp.float32), axis=0)
    weighted = jnp.einsum("bkec,bk->ecb", own_table, routing_weight, precision=PRECISE)
    moe_slice = jnp.einsum(
        "ecb,ecd->bd", weighted, back_experts.astype(jnp.float32), precision=PRECISE
    )
    moe_rows = lax.all_to_all(moe_slice, "tp", split_axis=0, concat_axis=1, tiled=True)
    residual_rows = lax.dynamic_slice_in_dim(hidden_sum, lane_index * per_lane, per_lane, 0)
    layer_out = (residual_rows + moe_rows + jax.nn.sigmoid(dense_gate_offset) * dense_sum).astype(
        jnp.bfloat16
    )
    return (layer_out, next_state)


def proj_state_kernel(count, *refs):
    sources, refs = refs[:count], refs[count:]
    state_ref, next_ref, part_ref, base_ref, wext_ref = refs[:5]
    held, (sbuf, nbuf, arg_sem, in_sem, out_sem) = refs[5 : 5 + count], refs[5 + count :]
    (tokens_ref, gain_ref, wr_ref, wk_ref, wv_ref, wd_ref, doff_ref, coff_ref, cfac_ref,
     own_ref, hgain_ref, routes_ref, rweight_ref, wo_ref) = held
    pulls = [
        pltpu.make_async_copy(src, dst, arg_sem.at[i])
        for i, (src, dst) in enumerate(zip(sources, held))
    ]
    for pull in pulls:
        pull.start()
    seqs, width = tokens_ref.shape
    heads = state_ref.shape[1]
    lanes = part_ref.shape[0]
    rows = part_ref.shape[1]
    loads = [
        pltpu.make_async_copy(state_ref.at[:, h, :], sbuf.at[h], in_sem.at[h]) for h in range(heads)
    ]
    for load in loads:
        load.start()
    f32, bf16 = jnp.float32, jnp.bfloat16
    for pull in pulls[:2]:
        pull.wait()
    toks = tokens_ref[...].astype(f32)
    normed = (
        toks * lax.rsqrt(jnp.mean(toks * toks, axis=-1, keepdims=True) + 1e-06) * gain_ref[...]
    ).astype(bf16)
    pulls[2].wait()
    recept = jnp.dot(normed, wr_ref[...], preferred_element_type=f32)
    pulls[3].wait()
    keys = jnp.dot(normed, wk_ref[...], preferred_element_type=f32)
    pulls[4].wait()
    values = jnp.dot(normed, wv_ref[...], preferred_element_type=f32)
    pulls[5].wait()
    logits = jnp.dot(normed, wd_ref[...], preferred_element_type=f32)
    for pull in pulls[6:]:
        pull.wait()
    decay = jnp.exp(-jnp.exp(doff_ref[...] + logits))
    rate = jax.nn.sigmoid(coff_ref[...] + cfac_ref[...] * keys)
    key_in = keys * rate
    own_prod = recept * key_in * own_ref[...]
    hgain = jnp.broadcast_to(hgain_ref[...], keys.shape)
    pair = 2 * HEAD_WIDTH
    lane = lax.broadcasted_iota(jnp.int32, (seqs, pair), 1)
    low = lane < HEAD_WIDTH
    half_r = lax.broadcasted_iota(jnp.int32, (pair, pair), 0) // HEAD_WIDTH
    half_c = lax.broadcasted_iota(jnp.int32, (pair, pair), 1) // HEAD_WIDTH
    ones_block = (half_r == half_c).astype(f32).astype(bf16)

    def group_sum(block):
        high = block.astype(bf16)
        rest = (block - high.astype(f32)).astype(bf16)
        return jnp.dot(high, ones_block, preferred_element_type=f32) + jnp.dot(
            rest, ones_block, preferred_element_type=f32
        )

    def doubled(full, h):
        chunk = full[:, (h // 2) * pair : (h // 2 + 1) * pair]
        turned = pltpu.roll(chunk, HEAD_WIDTH, 1)
        return jnp.where(low, chunk, turned) if h % 2 == 0 else jnp.where(low, turned, chunk)

    chunks = state_ref.shape[2] // pair
    step = 8
    outs, stores = [], []
    for h in range(heads):
        k2, r2, v2 = doubled(keys, h), doubled(recept, h), doubled(values, h)
        d2, kin2, rate2 = doubled(decay, h), doubled(key_in, h), doubled(rate, h)
        unit = (
            k2
            * lax.rsqrt(jnp.mean(k2 * k2, axis=-1, keepdims=True) + 1e-06)
            * HEAD_WIDTH ** (-0.5)
        )
        own_total = 0.5 * jnp.sum(doubled(own_prod, h), axis=-1, keepdims=True)

        def many(block):
            return jnp.concatenate([block] * step, axis=0)

        unit_m, back_m, dec_m = many(unit), many(unit * rate2), many(d2)
        kin_m, rec_m = many(kin2), many(r2)
        loads[h].wait()
        acc = jnp.zeros((seqs, pair), f32)
        for q in range(0, chunks, step):
            picks = [(lane == 2 * j) | (lane == HEAD_WIDTH + 2 * j + 1) for j in range(q, q + step)]
            old = jnp.concatenate(
                [sbuf[h, :, j * pair : (j + 1) * pair] for j in range(q, q + step)], axis=0
            )
            removed = group_sum(old * unit_m)
            spread_v = group_sum(jnp.concatenate([jnp.where(p, v2, 0.0) for p in picks], axis=0))
            new = old * dec_m - removed * back_m + spread_v * kin_m
            for i in range(step):
                nbuf[h, :, (q + i) * pair : (q + i + 1) * pair] = new[i * seqs : (i + 1) * seqs]
            read = group_sum(new * rec_m)
            for i in range(step):
                acc = acc + jnp.where(picks[i], read[i * seqs : (i + 1) * seqs], 0.0)
        store = pltpu.make_async_copy(nbuf.at[h], next_ref.at[:, h, :], out_sem.at[h])
        store.start()
        stores.append(store)
        y = acc + pltpu.roll(acc, HEAD_WIDTH, 1)
        center = y - jnp.mean(y, axis=-1, keepdims=True)
        var = jnp.mean(center * center, axis=-1, keepdims=True)
        outs.append(center * lax.rsqrt(var + 0.00064) * doubled(hgain, h) + own_total * v2)
    merged = jnp.concatenate(
        [jnp.where(low, outs[h], outs[h + 1]) for h in range(0, heads, 2)], axis=1
    ).astype(bf16)
    part = jnp.dot(merged, wo_ref[...], preferred_element_type=f32)
    me_lane = lax.axis_index("tp")
    base = jnp.zeros((rows, width), f32)
    for i in range(lanes):
        mine = part[i * rows : (i + 1) * rows]
        part_ref[i] = mine.astype(bf16)
        base = jnp.where(me_lane == i, mine + toks[i * rows : (i + 1) * rows], base)
    base_ref[...] = base
    start = lax.axis_index("ep") * seqs + me_lane * rows

    def picked_column(ref, k, first):
        spot = lax.broadcasted_iota(jnp.int32, (rows, ref.shape[1]), 1)
        wanted = spot == first + lax.broadcasted_iota(jnp.int32, spot.shape, 0)
        entries = ref[k : k + 1, :].astype(f32)
        return jnp.sum(jnp.where(wanted, entries, 0.0), axis=-1, keepdims=True)

    column = lax.broadcasted_iota(jnp.int32, (rows, 128), 1) % 64
    column = column.astype(f32)
    table = jnp.zeros((rows, 128), f32)
    for k in range(routes_ref.shape[0]):
        expert = picked_column(routes_ref, k, start)
        table = table + jnp.where(
            column == expert, picked_column(rweight_ref, k, me_lane * rows), 0.0
        )
    wext_ref[...] = table
    for store in stores:
        store.wait()


def exchange_kernel(
    groups, lanes,
    part_ref, base_ref, wext_ref, gain_hbm, goff_hbm,
    eg_hbm, eu_hbm, ed_hbm, dg_hbm, du_hbm, dd_hbm,
    out_ref,
    eg, eu, ed, dg, du, dd, gain, goff, hid_rows, p_in, xs, flat, hid, dens, ys, y_in, z_in, v_out, v_in,
    w_sem, s1, r1, sz, rz, st, rt, sc, rc, sa, ra, sb, rb, sv, rv,
):
    f32, bf16 = jnp.float32, jnp.bfloat16
    rows, width = base_ref.shape
    zs = groups // 2
    me_g, me_l = lax.axis_index("ep"), lax.axis_index("tp")
    core, me_z = lax.rem(me_g, 2), me_g // 2
    partner = (me_g + 1 - 2 * core, me_l)

    def lane_peer(d):
        return (me_g, lax.rem(me_l + d + lanes, lanes))

    def z_peer(d):
        return (lax.rem(me_z + d + zs, zs) * 2 + core, me_l)

    def send(src, dst, ssem, rsem, peer):
        copy = pltpu.make_async_remote_copy(
            src_ref=src, dst_ref=dst, send_sem=ssem, recv_sem=rsem, device_id=peer,
            device_id_type=pl.DeviceIdType.MESH,
        )
        copy.start()
        return copy

    pulls = [
        pltpu.make_async_copy(src, dst, w_sem.at[i])
        for i, (src, dst) in enumerate(
            [(gain_hbm, gain), (goff_hbm, goff), (dg_hbm, dg), (du_hbm, du), (dd_hbm, dd), (eg_hbm.at[0], eg), (eu_hbm.at[0], eu),
             (ed_hbm.at[0], ed)]
        )
    ]
    for pull in pulls:
        pull.start()
    barrier = pltpu.get_barrier_semaphore()
    peers = [lane_peer(d) for d in range(1, lanes)] + [z_peer(d) for d in range(1, zs)] + [partner]
    for peer in peers:
        pl.semaphore_signal(barrier, inc=1, device_id=peer, device_id_type=pl.DeviceIdType.MESH)
    pl.semaphore_wait(barrier, len(peers))
    sent = []
    firsts = []
    for d in range(1, lanes):
        target = lax.rem(me_l + lanes - d, lanes)
        firsts.append(
            send(part_ref.at[target], p_in.at[d - 1], s1.at[d - 1], r1.at[d - 1], (me_g, target))
        )
    hidden = base_ref[...]
    for d, copy in enumerate(firsts):
        copy.wait_recv()
        hidden = hidden + p_in[d].astype(f32)
    sent += firsts
    hid_rows[...] = hidden
    for pull in pulls[:2]:
        pull.wait()
    normed = hidden * lax.rsqrt(jnp.mean(hidden * hidden, axis=-1, keepdims=True) + 1e-06)
    xs[0, 0, 0, :, :width] = (normed * gain[...]).astype(bf16)
    table = wext_ref[...]
    high = table.astype(bf16).astype(f32)
    first_half = lax.broadcasted_iota(jnp.int32, table.shape, 1) < 64
    xs[0, 0, 0, :, width:] = jnp.where(first_half, high, table - high).astype(bf16)
    hold_z, hold_t, hold_c = {}, {}, {}
    for d in range(1, zs):
        hold_z[d] = send(xs.at[0, 0, 0], xs.at[0, 0, d], sz.at[d - 1], rz.at[d - 1], z_peer(d))

    def to_partner(d, q):
        i = d * zs + q
        hold_c[d, q] = send(xs.at[0, d, q], xs.at[1, d, q], sc.at[i], rc.at[i], partner)

    def to_lanes(q):
        to_partner(0, q)
        for d in range(1, lanes):
            i = (d - 1) * zs + q
            hold_t[d, q] = send(xs.at[0, 0, q], xs.at[0, d, q], st.at[i], rt.at[i], lane_peer(d))

    to_lanes(0)
    for q in range(1, zs):
        hold_z[q].wait_recv()
        to_lanes(q)
    block = 2 * zs * rows

    def gathered(d):
        return xs[:, d].astype(f32).reshape(block, width + 128)

    for q in range(zs):
        hold_c[0, q].wait_recv()
    mine = gathered(0)
    flat[0:block] = mine.astype(bf16)
    own_rows = mine[:, :width].astype(bf16)
    for pull in pulls[2:5]:
        pull.wait()
    across = (((1,), (1,)), ((), ()))
    gate = lax.dot_general(own_rows, dg[...], across, preferred_element_type=f32)
    up = lax.dot_general(own_rows, du[...], across, preferred_element_type=f32)
    mixed = (jax.nn.silu(gate) * up).astype(bf16)
    dens[...] = jnp.dot(mixed, dd[...], preferred_element_type=f32) * jax.nn.sigmoid(goff[...])
    for q in range(zs):
        for d in range(1, lanes):
            hold_t[d, q].wait_recv()
            to_partner(d, q)
    for d in range(1, lanes):
        for q in range(zs):
            hold_c[d, q].wait_recv()
        flat[d * block : (d + 1) * block] = gathered(d).astype(bf16)
    for pull in pulls[5:]:
        pull.wait()
    tile = 256

    @pl.loop(0, eg.shape[1] // tile)
    def _(n):
        cols = pl.ds(pl.multiple_of(n * tile, tile), tile)
        left = flat[:, :width]
        gated = jnp.dot(left, eg[:, cols], preferred_element_type=f32)
        raised = jnp.dot(left, eu[:, cols], preferred_element_type=f32)
        hid[:, cols] = (jax.nn.silu(gated) * raised).astype(bf16)

    tail = flat[:, width:].astype(f32)
    picked = lax.broadcasted_iota(jnp.int32, tail.shape, 1) % 64 == me_g
    scale = jnp.sum(jnp.where(picked, tail, 0.0), axis=-1, keepdims=True)
    pieces, wide = ys.shape[0], ys.shape[-1]
    to_core, to_lane, to_z = [], [], []

    def pass_on(n):
        to_core[n].wait_recv()
        own = []
        for d in range(1, lanes):
            ys[n, 0, d] = (ys[n, 0, d].astype(f32) + y_in[n, d].astype(f32)).astype(bf16)
            i = n * (lanes - 1) + d - 1
            own.append(
                send(ys.at[n, 0, d], z_in.at[n, d - 1], sb.at[i], rb.at[i], lane_peer(-d))
            )
        to_lane.append(own)

    for n in range(pieces):
        cols = slice(n * wide, (n + 1) * wide)
        made = jnp.dot(hid[...], ed[:, cols], preferred_element_type=f32) * scale
        for d in range(lanes):
            piece = made[d * block : (d + 1) * block]
            if d == 0:
                piece = piece + dens[:, cols]
            ys[n, :, d] = piece.reshape(2, zs, rows, wide).astype(bf16)
        to_core.append(send(ys.at[n, 1], y_in.at[n], sa.at[n], ra.at[n], partner))
        if n > 0:
            pass_on(n - 1)
    pass_on(pieces - 1)
    for n in range(pieces):
        cols = slice(n * wide, (n + 1) * wide)
        total = ys[n, 0, 0].astype(f32) + y_in[n, 0].astype(f32)
        for d in range(1, lanes):
            to_lane[n][d - 1].wait_recv()
            total = total + z_in[n, d - 1].astype(f32)
        v_out[n] = total.astype(bf16)
        own = []
        for d in range(1, zs):
            i = n * (zs - 1) + d - 1
            own.append(
                send(v_out.at[n, d], v_in.at[n, d - 1], sv.at[i], rv.at[i], z_peer(-d))
            )
        to_z.append(own)
        hid_rows[:, cols] = hid_rows[:, cols] + total[0]
    for n in range(pieces):
        cols = slice(n * wide, (n + 1) * wide)
        result = hid_rows[:, cols]
        for d, copy in enumerate(to_z[n]):
            copy.wait_recv()
            result = result + v_in[n, d].astype(f32)
        out_ref[:, cols] = result.astype(bf16)
    sent += list(hold_z.values()) + list(hold_t.values()) + list(hold_c.values())
    sent += to_core
    for own in to_lane + to_z:
        sent += own
    for copy in sent:
        copy.wait_send()


def fused(
    tokens, recurrent_head_state, first_norm_gain, receptance_matrix, key_matrix, value_matrix,
    decay_matrix, decay_offset, correction_offset, correction_key_factor, own_term_weight,
    head_norm_gain, output_matrix, second_norm_gain, routing, routing_weight, expert_gate_weight,
    expert_up_weight, expert_down_weight, dense_gate_weight, dense_up_weight, dense_down_weight,
    dense_gate_offset,
):
    f32, bf16 = jnp.float32, jnp.bfloat16
    seqs, width = tokens.shape
    heads, flat_width = recurrent_head_state.shape[1:]
    groups, lanes = lax.axis_size("ep"), lax.axis_size("tp")
    rows, zs = seqs // lanes, groups // 2
    handed = lanes * rows * width * 2 + rows * width * 4 + rows * 128 * 4
    grant = VMEM_BYTES - handed
    vmem = pl.BlockSpec(memory_space=pltpu.VMEM)
    anywhere = pl.BlockSpec(memory_space=pltpu.HBM)
    dma = pltpu.SemaphoreType.DMA

    def row(vector):
        return vector.reshape(1, -1)

    operands = (
        tokens, row(first_norm_gain), receptance_matrix, key_matrix, value_matrix, decay_matrix,
        row(decay_offset), row(correction_offset), row(correction_key_factor),
        row(own_term_weight), row(head_norm_gain), routing.T, routing_weight.T, output_matrix,
    )
    count = len(operands)
    next_state, part, base, table = pl.pallas_call(
        functools.partial(proj_state_kernel, count),
        out_shape=(
            jax.ShapeDtypeStruct(recurrent_head_state.shape, f32),
            jax.ShapeDtypeStruct((lanes, rows, width), bf16),
            jax.ShapeDtypeStruct((rows, width), f32),
            jax.ShapeDtypeStruct((rows, 128), f32),
        ),
        in_specs=[anywhere] * (count + 1),
        out_specs=(anywhere, vmem, vmem, vmem),
        scratch_shapes=[pltpu.VMEM(operand.shape, operand.dtype) for operand in operands]
        + [
            pltpu.VMEM((heads, seqs, flat_width), f32),
            pltpu.VMEM((heads, seqs, flat_width), f32),
            dma((count,)),
            dma((heads,)),
            dma((heads,)),
        ],
        compiler_params=pltpu.CompilerParams(vmem_limit_bytes=grant),
        name="proj_state",
    )(*operands, recurrent_head_state)
    hidden_units = expert_gate_weight.shape[2]
    pieces = 4
    wide = width // pieces
    total = groups * seqs
    layer_out = pl.pallas_call(
        functools.partial(exchange_kernel, groups, lanes),
        out_shape=jax.ShapeDtypeStruct((rows, width), bf16),
        in_specs=[vmem] * 3 + [anywhere] * 8,
        out_specs=vmem,
        scratch_shapes=[
            pltpu.VMEM(expert_gate_weight.shape[1:], bf16),
            pltpu.VMEM(expert_up_weight.shape[1:], bf16),
            pltpu.VMEM(expert_down_weight.shape[1:], bf16),
            pltpu.VMEM(dense_gate_weight.shape[::-1], bf16),
            pltpu.VMEM(dense_up_weight.shape[::-1], bf16),
            pltpu.VMEM(dense_down_weight.shape, bf16),
            pltpu.VMEM((1, width), f32),
            pltpu.VMEM((1, width), f32),
            pltpu.VMEM((rows, width), f32),
            pltpu.VMEM((lanes - 1, rows, width), bf16),
            pltpu.VMEM((2, lanes, zs, rows, width + 128), bf16),
            pltpu.VMEM((total, width + 128), bf16),
            pltpu.VMEM((total, hidden_units), bf16),
            pltpu.VMEM((2 * zs * rows, width), f32),
            pltpu.VMEM((pieces, 2, lanes, zs, rows, wide), bf16),
            pltpu.VMEM((pieces, lanes, zs, rows, wide), bf16),
            pltpu.VMEM((pieces, lanes - 1, zs, rows, wide), bf16),
            pltpu.VMEM((pieces, zs, rows, wide), bf16),
            pltpu.VMEM((pieces, zs - 1, rows, wide), bf16),
            dma((8,)),
            dma((lanes - 1,)), dma((lanes - 1,)),
            dma((zs - 1,)), dma((zs - 1,)),
            dma(((lanes - 1) * zs,)), dma(((lanes - 1) * zs,)),
            dma((lanes * zs,)), dma((lanes * zs,)),
            dma((pieces,)), dma((pieces,)),
            dma((pieces * (lanes - 1),)), dma((pieces * (lanes - 1),)),
            dma((pieces * (zs - 1),)), dma((pieces * (zs - 1),)),
        ],
        compiler_params=pltpu.CompilerParams(
            collective_id=0, has_side_effects=True, vmem_limit_bytes=grant - rows * width * 2
        ),
        name="exchange",
    )(
        part, base, table, row(second_norm_gain), row(dense_gate_offset), expert_gate_weight,
        expert_up_weight, expert_down_weight, dense_gate_weight.T, dense_up_weight.T,
        dense_down_weight,
    )
    return (layer_out, next_state)


def choose(tokens, recurrent_head_state, *rest):
    groups, lanes = lax.axis_size("ep"), lax.axis_size("tp")
    rows, heads = tokens.shape[0] // lanes, recurrent_head_state.shape[1]
    experts_here = rest[14].shape[0]
    fits = (
        rows % 8 == 0 and heads % 2 == 0 and groups % 2 == 0 and groups > 2 and lanes > 1
        and groups <= 64 and experts_here == 1
    )
    return (fused if fits else local)(tokens, recurrent_head_state, *rest)


def solution(mesh):
    return jax.shard_map(
        choose,
        mesh=mesh,
        in_specs=(
            P("ep", None),
            P("ep", "tp", None),
            P(),
            P(None, "tp"),
            P(None, "tp"),
            P(None, "tp"),
            P(None, "tp"),
            P("tp"),
            P("tp"),
            P("tp"),
            P("tp"),
            P("tp"),
            P("tp", None),
            P(),
            P(),
            P("ep", None),
            P("ep", None, "tp"),
            P("ep", None, "tp"),
            P("ep", "tp", None),
            P(None, "ep"),
            P(None, "ep"),
            P("ep", None),
            P(),
        ),
        out_specs=(P(("ep", "tp"), None), P("ep", "tp", None)),
        check_vma=False,
    )
```
